32 devices in a mesh: grp: 2 (over y), ra: 4 (over z), cb: 4 (over x, core).
Axes of the slice: x: 2, y: 2, z: 4, core: 2. Of those that a mesh axis runs over, the one named last changes fastest.
Arguments:
- tokens: bfloat16 [512, 4096], P('grp', 'cb'), parts along dimension 0, may hold values from -50 to 50
- norm_gains: float32 [3, 4096], P(None, 'cb'), may hold values from 0.1 to 1.9
- gate_weight: float32 [2, 4096, 11264], P(None, 'cb', 'ra'), may hold values from -0.09375 to 0.09375
- value_weight: float32 [2, 4096, 11264], P(None, 'cb', 'ra'), may hold values from -0.09375 to 0.09375
- gate_scale: float32 [2, 11264], P(None, 'ra'), may hold values from 0.3 to 3
- value_scale: float32 [2, 11264], P(None, 'ra'), may hold values from 0.3 to 3
- conv_gate: float32 [2, 3, 11264], P(None, None, 'ra'), may hold values from -3 to 3
- conv_value: float32 [2, 3, 11264], P(None, None, 'ra'), may hold values from -3 to 3
- down_weight: float32 [2, 11264, 4096], P(None, 'ra', 'cb'), may hold values from -0.07537784 to 0.07537784
- down_scale: float32 [2, 4096], P(None, 'cb'), may hold values from 0.3 to 3
Outputs:
- normed_out: bfloat16 [512, 4096], P('grp', 'cb'), parts along dimension 0
The draws below stay inside these ranges and needn't reach their ends.
There are 2 independent parts, one for each index of `grp`. The reference program is written for one: setup_inputs(seed, part) draws one part's arguments, and reference() takes and returns one part's arrays. A program takes and returns all parts, laid end to end along the dimension named above; an argument that names none is the same for every part. Nothing has to cross between parts.
All inputs are finite; a program needn't handle non-finite values.
Results may differ from the reference program's by a relative error of at most 0.012.
The reference program's roundings to bfloat16 on the way count: a program that leaves them out, or rounds other values in their place, can miss the bound.
Values may be sent and summed in bfloat16 or wider, within the bound.
A program may use at most 192 MiB of HBM per device.

```python
import math
import jax
import jax.numpy as jnp
from jax import lax

D = 4096
FF = 11264
TOK = 256
LAYERS = 2
TAPS = 3


def draw_tokens(key, part):
    key_values = jax.random.fold_in(key, 11)
    key_rows = jax.random.fold_in(key, 12)
    col_position = jnp.arange(D, dtype=jnp.float32) / D
    col_scale = 10.0 ** (col_position - 0.5)
    row_scale = 10.0 ** (jax.random.uniform(key_rows, (TOK, 1), jnp.float32) - 0.5)
    values = jnp.clip(jax.random.normal(key_values, (TOK, D), jnp.float32), -5.0, 5.0)
    return (values * row_scale * col_scale).astype(jnp.bfloat16)


def draw_down_weight(key, part):
    key_base = jax.random.fold_in(key, 21)
    unit = FF ** (-0.5)
    base = jnp.clip(jax.random.normal(key_base, (LAYERS, FF, D), jnp.float32), -6.0, 6.0) * unit
    values = base
    return values.astype(jnp.float32)


def steps_of(rng, dims, shards, least, largest):
    loudness = 1.0
    for axis_at, parts in shards:
        heights = jax.random.uniform(jax.random.fold_in(jax.random.fold_in(rng, 6), axis_at), (parts,), jnp.float32, least / len(shards), largest / len(shards))
        loudness = loudness * jnp.repeat(jnp.exp(heights), dims[axis_at] // parts).reshape((-1,) + (1,) * (len(dims) - 1 - axis_at))
    return loudness


def centred(own_key, dims, scale, bound, shards=(), kind=jnp.bfloat16):
    drawn = jax.random.normal(own_key, dims, jnp.float32) * scale
    if len(shards) > 0:
        drawn = steps_of(own_key, dims, shards, -0.22, 0.18) * drawn
    return jnp.clip(drawn, min=-bound, max=bound).astype(kind)


def setup_inputs(seed: int = 0, part: int = 0) -> dict:
    streams_of = jax.random.split(jax.random.key(seed), 11)
    own_keys = jax.random.split(jax.random.fold_in(streams_of[10], part), 11)
    return {
        "tokens": draw_tokens(jax.random.fold_in(jax.random.fold_in(streams_of[10], part), 71), part),
        "norm_gains": jnp.clip(1.0 + 0.18 * jax.random.normal(streams_of[1], (LAYERS + 1, D), jnp.float32), 0.1, 1.9),
        "gate_weight": centred(streams_of[2], (LAYERS, D, FF), D ** -0.5, 0.09375, ((1, 4), (2, 4)), jnp.float32),
        "value_weight": centred(streams_of[3], (LAYERS, D, FF), D ** -0.5, 0.09375, ((1, 4), (2, 4)), jnp.float32),
        "gate_scale": jnp.clip(jnp.exp(math.log(3.0) - 2.3025851 * jax.random.uniform(streams_of[4], (LAYERS, FF), jnp.float32) ** steps_of(streams_of[4], (LAYERS, FF), ((1, 4),), -0.2, 0.2)), 0.3, 3.0),
        "value_scale": jnp.clip(jnp.exp(math.log(3.0) - 2.3025851 * jax.random.uniform(streams_of[5], (LAYERS, FF), jnp.float32) ** steps_of(streams_of[5], (LAYERS, FF), ((1, 4),), -0.2, 0.2)), 0.3, 3.0),
        "conv_gate": centred(streams_of[6], (LAYERS, TAPS, FF), 0.6, 3.0, ((2, 4),), jnp.float32),
        "conv_value": centred(streams_of[7], (LAYERS, TAPS, FF), 0.6, 3.0, ((2, 4),), jnp.float32),
        "down_weight": draw_down_weight(jax.random.fold_in(streams_of[10], 71), part),
        "down_scale": jnp.clip(jnp.exp(math.log(3.0) - 2.3025851 * jax.random.uniform(streams_of[9], (LAYERS, D), jnp.float32) ** steps_of(streams_of[9], (LAYERS, D), ((1, 4),), -0.2, 0.2)), 0.3, 3.0),
    }


epsilon = 1e-06
residual_weight = 0.5

def rms_scale(values):
    return lax.rsqrt(lax.optimization_barrier(jnp.mean(values * values, axis=1, keepdims=True)) + epsilon)

def causal_taps(projected, tap_weights):
    tap_count = tap_weights.shape[0]
    row_count = projected.shape[0]
    padded = jnp.pad(projected, ((tap_count - 1, 0), (0, 0)))
    result = jnp.zeros_like(projected)
    for tap_idx in range(tap_count):
        result = result + padded[tap_idx:tap_idx + row_count] * tap_weights[tap_idx]
    return result

def reference(tokens, norm_gains, gate_weight, value_weight, gate_scale, value_scale, conv_gate, conv_value, down_weight, down_scale):
    current = tokens
    for layer_idx in range(LAYERS):
        state_wide = current.astype(jnp.float32)
        inverse = rms_scale(state_wide)
        scaled = (state_wide * norm_gains[layer_idx]).astype(jnp.bfloat16)
        gate_pre = inverse * gate_scale[layer_idx] * jnp.dot(scaled, gate_weight[layer_idx].astype(jnp.bfloat16), preferred_element_type=jnp.float32)
        value_pre = inverse * value_scale[layer_idx] * jnp.dot(scaled, value_weight[layer_idx].astype(jnp.bfloat16), preferred_element_type=jnp.float32)
        hidden = (jax.nn.gelu(causal_taps(gate_pre, conv_gate[layer_idx]), approximate=True) * causal_taps(value_pre, conv_value[layer_idx])).astype(jnp.bfloat16)
        down_total = jnp.dot(hidden, down_weight[layer_idx].astype(jnp.bfloat16), preferred_element_type=jnp.float32)
        current = (residual_weight * state_wide + down_scale[layer_idx] * down_total).astype(jnp.bfloat16)
    state_wide = current.astype(jnp.float32)
    return (state_wide * rms_scale(state_wide) * norm_gains[LAYERS]).astype(jnp.bfloat16)
```

```python
import functools

import jax
import jax.numpy as jnp
from jax import lax
from jax.experimental import pallas as pl
from jax.experimental.pallas import tpu as pltpu
from jax.sharding import PartitionSpec as P

epsilon = 1e-06
residual_weight = 0.5


def causal_taps(projected, tap_weights):
    tap_count = tap_weights.shape[0]
    row_count = projected.shape[0]
    padded = jnp.pad(projected, ((tap_count - 1, 0), (0, 0)))
    result = jnp.zeros_like(projected)
    for tap_idx in range(tap_count):
        result = result + padded[tap_idx : tap_idx + row_count] * tap_weights[tap_idx]
    return result


def row_inverse(state_wide, model_width):
    squares = lax.psum(jnp.sum(state_wide * state_wide, axis=1, keepdims=True), "cb")
    return lax.rsqrt(squares / model_width + epsilon)


def on_device(
    tokens,
    norm_gains,
    gate_weight,
    value_weight,
    gate_scale,
    value_scale,
    conv_gate,
    conv_value,
    down_weight,
    down_scale,
):
    model_width = lax.axis_size("cb") * tokens.shape[1]
    layer_count = gate_weight.shape[0]
    current = tokens
    for layer_idx in range(layer_count):
        state_wide = current.astype(jnp.float32)
        inverse = row_inverse(state_wide, model_width)
        scaled = (state_wide * norm_gains[layer_idx]).astype(jnp.bfloat16)
        gate_part = jnp.dot(
            scaled, gate_weight[layer_idx].astype(jnp.bfloat16), preferred_element_type=jnp.float32
        )
        value_part = jnp.dot(
            scaled, value_weight[layer_idx].astype(jnp.bfloat16), preferred_element_type=jnp.float32
        )
        gate_sum, value_sum = (
            lax.psum_scatter(gate_part, "cb", scatter_dimension=1, tiled=True),
            lax.psum_scatter(value_part, "cb", scatter_dimension=1, tiled=True),
        )
        share_cols = gate_sum.shape[1]
        first_col = lax.axis_index("cb") * share_cols
        gate_cols = lax.dynamic_slice_in_dim(gate_scale[layer_idx], first_col, share_cols, 0)
        value_cols = lax.dynamic_slice_in_dim(value_scale[layer_idx], first_col, share_cols, 0)
        gate_taps = lax.dynamic_slice_in_dim(conv_gate[layer_idx], first_col, share_cols, 1)
        value_taps = lax.dynamic_slice_in_dim(conv_value[layer_idx], first_col, share_cols, 1)
        gate_pre = inverse * gate_cols * gate_sum
        value_pre = inverse * value_cols * value_sum
        hidden = (
            jax.nn.gelu(causal_taps(gate_pre, gate_taps), approximate=True)
            * causal_taps(value_pre, value_taps)
        ).astype(jnp.bfloat16)
        hidden = lax.all_gather(hidden, "cb", axis=1, tiled=True)
        partial_value = jnp.dot(
            hidden, down_weight[layer_idx].astype(jnp.bfloat16), preferred_element_type=jnp.float32
        )
        down_total = lax.psum(partial_value, "ra")
        current = (residual_weight * state_wide + down_scale[layer_idx] * down_total).astype(
            jnp.bfloat16
        )
    state_wide = current.astype(jnp.float32)
    inverse = row_inverse(state_wide, model_width)
    return (state_wide * inverse * norm_gains[layer_count]).astype(jnp.bfloat16)


CORES = 2
LANES = 128
GROUP = 64
RING = 13
WIDE_SLOTS = 16
DOWN_SLOTS = 16
FIRST_LOADS = 6
DOWN_LAG = 3
BUBBLES = 3
PAIR_SUM, GATED, PAIR_GATHER, DOWN = 2, 5, 8, 10
Z_SUM, Z_GATHER, Z_SCALE = 6, 12, 13


def fused_kernel(
    ra_count,
    cb_count,
    tokens,
    gains,
    gate_hbm,
    value_hbm,
    gate_scale,
    value_scale,
    conv_gate,
    conv_value,
    down_hbm,
    down_scale,
    out,
    wide_weight,
    down_weight,
    current,
    scaled,
    inverse,
    padded,
    carry,
    pair_send,
    pair_recv,
    pair_own,
    x_send,
    x_recv,
    hidden,
    acc,
    z_send,
    z_recv,
    z_own,
    sq_send,
    sq_recv,
    wide_sem,
    down_sem,
    pair_ss,
    pair_rs,
    x_ss,
    x_rs,
    hx_ss,
    hx_rs,
    hp_ss,
    hp_rs,
    z_ss,
    z_rs,
    c_ss,
    c_rs,
    sq_ss,
    sq_rs,
):
    f32, bf16 = jnp.float32, jnp.bfloat16
    layers = gate_hbm.shape[0]
    groups = tokens.shape[0]
    rows = tokens.shape[1]
    width = tokens.shape[2]
    x_count = cb_count // CORES
    chunk_cols = x_count * LANES
    chunks = gate_hbm.shape[2] // chunk_cols
    pairs = pl.cdiv(chunks, CORES)
    taps = conv_gate.shape[0]
    model_width = width * cb_count
    z_block = rows // ra_count
    per_layer = groups * pairs
    period = per_layer + BUBBLES
    last_item = layers * period - BUBBLES
    all_groups = groups + (BUBBLES > 0)
    streamed = layers * chunks

    me_cb = lax.axis_index("cb")
    me_ra = lax.axis_index("ra")
    me_x, me_core = lax.div(me_cb, CORES), lax.rem(me_cb, CORES)
    partner = me_x * CORES + (1 - me_core)

    def others(count, me):
        return [lax.rem(me + step, count) for step in range(1, count)]

    def remote(src, dst, send, recv, axis, index):
        return pltpu.make_async_remote_copy(
            src_ref=src,
            dst_ref=dst,
            send_sem=send,
            recv_sem=recv,
            device_id={axis: index},
            device_id_type=pl.DeviceIdType.MESH,
        )

    cb_peers, ra_peers, x_peers = others(cb_count, me_cb), others(ra_count, me_ra), others(x_count, me_x)

    def cb_of(x_index):
        return x_index * CORES + me_core

    def place_of(n):
        layer = sum((jnp.asarray(n >= later * chunks).astype(jnp.int32) for later in range(1, layers)), 0)
        return layer, n - layer * chunks

    def wide_copies(n):
        (layer, chunk), slot = place_of(n), lax.rem(n, WIDE_SLOTS)
        cols = pl.ds(pl.multiple_of(chunk * chunk_cols, chunk_cols), chunk_cols)
        return (
            pltpu.make_async_copy(
                gate_hbm.at[layer, :, cols],
                wide_weight.at[slot, :, pl.ds(0, chunk_cols)],
                wide_sem.at[slot, 0],
            ),
            pltpu.make_async_copy(
                value_hbm.at[layer, :, cols],
                wide_weight.at[slot, :, pl.ds(chunk_cols, chunk_cols)],
                wide_sem.at[slot, 1],
            ),
        )

    def down_copies(n):
        (layer, chunk), slot = place_of(n), lax.rem(n, DOWN_SLOTS)
        cols = pl.ds(pl.multiple_of(chunk * chunk_cols, chunk_cols), chunk_cols)
        return (
            pltpu.make_async_copy(down_hbm.at[layer, cols, :], down_weight.at[slot], down_sem.at[slot]),
        )

    def start_copies(copies, n, limit):
        @pl.when(n < limit)
        def _():
            for copy in copies(n):
                copy.start()

    for n in range(min(FIRST_LOADS, streamed)):
        for copy in wide_copies(n):
            copy.start()

    barrier = pltpu.get_barrier_semaphore()
    for axis, count, me in (("cb", cb_count, me_cb), ("ra", ra_count, me_ra)):
        for peer in others(count, me):
            pl.semaphore_signal(
                barrier, inc=1, device_id={axis: peer}, device_id_type=pl.DeviceIdType.MESH
            )
    pl.semaphore_wait(barrier, cb_count + ra_count - 2)

    def pair_copy(slot):
        return remote(
            pair_send.at[slot], pair_recv.at[slot], pair_ss.at[slot], pair_rs.at[slot], "cb", partner
        )

    def x_copy(slot, peer, source):
        return remote(
            x_send.at[slot, peer],
            x_recv.at[slot, source],
            x_ss.at[slot, peer],
            x_rs.at[slot, source],
            "cb",
            cb_of(peer),
        )

    def hx_copy(slot, peer, source):
        place = hidden.at[slot, me_core * x_count + source]
        return remote(place, place, hx_ss.at[slot, peer], hx_rs.at[slot, source], "cb", cb_of(peer))

    def hp_copy(slot, core):
        place = hidden.at[slot, pl.ds(core * x_count, x_count)]
        return remote(place, place, hp_ss.at[slot], hp_rs.at[slot], "cb", partner)

    def z_copy(part, peer, source):
        return remote(
            z_send.at[part, peer],
            z_recv.at[part, source],
            z_ss.at[part, peer],
            z_rs.at[part, source],
            "ra",
            peer,
        )

    def c_copy(part, layer, group, peer, source):
        place = current.at[layer, group, source]
        return remote(place, place, c_ss.at[part, peer], c_rs.at[part, source], "ra", peer)

    def sq_copy(event, peer, source):
        return remote(
            sq_send.at[event], sq_recv.at[event, source], sq_ss.at[event, peer], sq_rs.at[event, source], "cb", peer
        )

    def scale_rows(layer, group):
        event = layer * groups + group
        wide = current[layer, group].reshape(rows, width).astype(f32)
        scaled[group] = (wide * gains[pl.ds(layer, 1), :]).astype(bf16).astype(f32)
        squares = jnp.broadcast_to(jnp.sum(wide * wide, axis=1, keepdims=True), (rows, LANES))
        sq_send[event] = jnp.concatenate([squares] * (LANES // rows), axis=0).T[:8]
        for peer in cb_peers:
            sq_copy(event, peer, me_cb).start()

    def finish_squares(layer, group):
        event = layer * groups + group
        total = sq_send[event]
        for peer in cb_peers:
            copy = sq_copy(event, peer, peer)
            copy.wait_send()
            copy.wait_recv()
            total = total + sq_recv[event, peer]
        row = lax.rsqrt(total / model_width + epsilon)
        inverse[group] = jnp.broadcast_to(row[:1], (LANES, LANES)).T[:rows]

    for group in range(groups):
        current[0, group] = tokens[group].reshape(ra_count, z_block, width)
        scale_rows(0, group)

    def when_full(pair, both, first_only):
        if chunks % CORES == 0:
            both()
        else:
            pl.when(pair < pairs - 1)(both)
            pl.when(pair == pairs - 1)(first_only)

    def when_owner(pair, fn):
        if chunks % CORES == 0:
            fn()
        else:
            pl.when((pair < pairs - 1) | (me_core == 0))(fn)

    def when_partner(pair, fn):
        if chunks % CORES == 0:
            fn()
        else:
            pl.when((pair < pairs - 1) | (me_core == 1))(fn)

    def project(layer, group, pair, slot):
        ordinal = group * pairs + pair
        first = layer * chunks + pair * CORES
        end = (layer + 1) * chunks

        @pl.when(layer == 0)
        def _():
            for n in range(CORES):
                start_copies(wide_copies, FIRST_LOADS + ordinal * CORES + n, min(WIDE_SLOTS, streamed))

            @pl.when(ordinal >= DOWN_LAG)
            def _():
                for n in range(CORES):
                    start_copies(down_copies, (ordinal - DOWN_LAG) * CORES + n, min(DOWN_SLOTS, streamed))

        @pl.when(group == 0)
        def _():
            for n in range(CORES):

                @pl.when(first + n < end)
                def _(n=n):
                    for copy in wide_copies(first + n):
                        copy.wait()

        def product_of(chunk_at):
            return jnp.dot(
                scaled[group], wide_weight[lax.rem(chunk_at, WIDE_SLOTS)], preferred_element_type=f32
            )

        def keep(chunk_at):
            product = product_of(chunk_at)
            for x in range(x_count):
                for kind in range(2):
                    at = kind * chunk_cols + x * LANES
                    pair_own[slot, x, :, kind * LANES : (kind + 1) * LANES] = product[:, at : at + LANES]

        def give(chunk_at):
            product = product_of(chunk_at)
            for x in range(x_count):
                for kind in range(2):
                    at = kind * chunk_cols + x * LANES
                    pair_send[slot, x, :, kind * LANES : (kind + 1) * LANES] = product[
                        :, at : at + LANES
                    ].astype(bf16)

        def both():
            give(first + 1 - me_core)
            pair_copy(slot).start()
            keep(first + me_core)

        def first_only():
            @pl.when(me_core == 0)
            def _():
                keep(first)

            @pl.when(me_core == 1)
            def _():
                give(first)
                pair_copy(slot).start()

        when_full(pair, both, first_only)

        @pl.when(group == groups - 1)
        def _():
            for n in range(CORES):

                @pl.when(first + n < end)
                def _(n=n):
                    start_copies(wide_copies, first + n + WIDE_SLOTS, streamed)

    def pair_sum(layer, group, pair, slot):
        when_partner(pair, lambda: pair_copy(slot).wait_send())

        def send():
            pair_copy(slot).wait_recv()
            for peer in x_peers:
                x_send[slot, peer] = (pair_own[slot, peer] + pair_recv[slot, peer].astype(f32)).astype(bf16)
                x_copy(slot, peer, me_x).start()

        when_owner(pair, send)

    def gated(layer, group, pair, slot):
        @pl.when(pair == 0)
        def _():
            finish_squares(layer, group)

        def unit():
            total = pair_own[slot, me_x] + pair_recv[slot, me_x].astype(f32)
            for peer in x_peers:
                copy = x_copy(slot, peer, peer)
                copy.wait_send()
                copy.wait_recv()
                total = total + x_recv[slot, peer].astype(f32)
            at = (pair * CORES + me_core) * chunk_cols
            cols = pl.ds(pl.multiple_of(at, chunk_cols), chunk_cols)
            one = pl.ds(layer, 1)

            def mine(values):
                kept = values[:, :LANES]
                for x in range(1, x_count):
                    kept = jnp.where(me_x == x, values[:, x * LANES : (x + 1) * LANES], kept)
                return kept

            scales = jnp.concatenate([mine(gate_scale[one, cols]), mine(value_scale[one, cols])], axis=1)
            weights = jnp.concatenate(
                [mine(conv_gate[:, layer, cols]), mine(conv_value[:, layer, cols])], axis=1
            )
            inv = inverse[group]
            pre = total * jnp.concatenate([inv, inv], axis=1) * scales
            before = carry[pair]
            padded[:8] = jnp.where(group == 0, jnp.zeros_like(before), before)
            padded[8:] = pre
            carry[pair] = pre[rows - 8 :]
            mixed = pre * weights[taps - 1 : taps]
            for tap in range(taps - 1):
                mixed = mixed + padded[pl.ds(8 - (taps - 1) + tap, rows), :] * weights[tap : tap + 1]
            hidden[slot, me_core * x_count + me_x] = (
                jax.nn.gelu(mixed[:, :LANES], approximate=True) * mixed[:, LANES:]
            ).astype(bf16)
            for peer in x_peers:
                hx_copy(slot, peer, me_x).start()

        when_owner(pair, unit)

    def pair_gather(layer, group, pair, slot):
        def forward():
            for peer in x_peers:
                hx_copy(slot, peer, me_x).wait_send()
                hx_copy(slot, peer, peer).wait_recv()
            hp_copy(slot, me_core).start()

        when_owner(pair, forward)

    def project_down(layer, group, pair, slot):
        first = layer * chunks + pair * CORES
        end = (layer + 1) * chunks

        @pl.when(group == 0)
        def _():
            for n in range(CORES):

                @pl.when(first + n < end)
                def _(n=n):
                    for copy in down_copies(first + n):
                        copy.wait()

        when_owner(pair, lambda: hp_copy(slot, me_core).wait_send())
        when_partner(pair, lambda: hp_copy(slot, 1 - me_core).wait_recv())

        def add(count):
            left = jnp.concatenate([hidden[slot, n] for n in range(count * x_count)], axis=1).astype(f32)
            right = jnp.concatenate(
                [down_weight[lax.rem(first + n, DOWN_SLOTS)] for n in range(count)], axis=0
            )
            product = jnp.dot(left, right, preferred_element_type=f32)
            before = acc[...]
            acc[...] = jnp.where(pair == 0, jnp.zeros_like(before), before) + product

        when_full(pair, lambda: add(CORES), lambda: add(1))

        @pl.when(group == groups - 1)
        def _():
            for n in range(CORES):

                @pl.when(first + n < end)
                def _(n=n):
                    start_copies(down_copies, first + n + DOWN_SLOTS, streamed)

        @pl.when(pair == pairs - 1)
        def _():
            part = layer * groups + group
            total = acc[...].reshape(ra_count, z_block, width)
            z_send[part] = total.astype(bf16)
            z_own[part] = acc[pl.ds(pl.multiple_of(me_ra * z_block, z_block), z_block), :]
            for peer in ra_peers:
                z_copy(part, peer, me_ra).start()

    def z_sum(layer, group, pair, slot):
        part = layer * groups + group
        total = z_own[part]
        for peer in ra_peers:
            copy = z_copy(part, peer, peer)
            copy.wait_send()
            copy.wait_recv()
            total = total + z_recv[part, peer].astype(f32)
        kept = residual_weight * current[layer, group, me_ra].astype(f32)
        current[layer + 1, group, me_ra] = (kept + down_scale[pl.ds(layer, 1), :] * total).astype(bf16)
        for peer in ra_peers:
            c_copy(part, layer + 1, group, peer, me_ra).start()

    def z_gather(layer, group, pair, slot):
        part = layer * groups + group
        for peer in ra_peers:
            c_copy(part, layer + 1, group, peer, me_ra).wait_send()
            c_copy(part, layer + 1, group, peer, peer).wait_recv()
        scale_rows(layer + 1, group)

    def z_scale(layer, group, pair, slot):
        @pl.when(layer == layers - 1)
        def _():
            finish_squares(layers, group)
            wide = current[layers, group].reshape(rows, width).astype(f32)
            inv = jnp.concatenate([inverse[group]] * (width // LANES), axis=1)
            out[group] = (wide * inv * gains[pl.ds(layers, 1), :]).astype(bf16)

    stages = (
        (DOWN + Z_SCALE, True, z_scale),
        (DOWN + Z_GATHER, True, z_gather),
        (DOWN + Z_SUM, True, z_sum),
        (PAIR_GATHER, False, pair_gather),
        (GATED, False, gated),
        (PAIR_SUM, False, pair_sum),
        (0, False, project),
        (DOWN, False, project_down),
    )

    delays = sorted({delay for delay, _, _ in stages})

    def started(delay):
        layer, rest = divmod(-delay, period)
        group, pair = (groups, rest - per_layer) if rest >= per_layer else divmod(rest, pairs)
        return tuple(jnp.int32(value) for value in (layer, group, pair, 0))

    def advanced(place):
        layer, group, pair, slot = place
        used = (layer >= 0) & (group < groups)
        slot = jnp.where(used, jnp.where(slot == RING - 1, 0, slot + 1), slot)
        wrap = pair + 1 == jnp.where(group == groups, BUBBLES, pairs)
        pair = jnp.where(wrap, 0, pair + 1)
        group = jnp.where(wrap, group + 1, group)
        next_layer = group == all_groups
        return jnp.where(next_layer, layer + 1, layer), jnp.where(next_layer, 0, group), pair, slot

    def step(index, places):
        for delay, at_end, stage in stages:
            place = places[delays.index(delay)]
            layer, group, pair, slot = place
            valid = (layer >= 0) & (layer < layers) & (group < groups)
            if at_end:
                valid = valid & (pair == pairs - 1)

            @pl.when(valid)
            def _(stage=stage, place=place):
                stage(*place)

        return tuple(advanced(place) for place in places)

    lax.fori_loop(0, last_item + DOWN + Z_SCALE, step, tuple(started(delay) for delay in delays))


def fits(ra_count, cb_count, tokens, gate_weight, conv_gate):
    rows, width = tokens.shape
    layers, _, units = gate_weight.shape
    if cb_count % CORES or cb_count <= CORES or ra_count < 2 or rows % GROUP or GROUP % (16 * ra_count):
        return False
    chunk_cols = cb_count // CORES * LANES
    if width % LANES or units % chunk_cols or units // chunk_cols < CORES or conv_gate.shape[1] > 9:
        return False
    chunks = units // chunk_cols
    pairs, groups = pl.cdiv(chunks, CORES), rows // GROUP
    weights = 4 * width * chunk_cols * (2 * WIDE_SLOTS + DOWN_SLOTS)
    return (
        chunks <= min(WIDE_SLOTS, DOWN_SLOTS)
        and (groups - 1) * pairs + 1 + BUBBLES >= DOWN + Z_GATHER
        and weights + 4 * rows * width * 12 <= 60 * 1024 * 1024
    )


def on_device_any(ra_count, cb_count, *args):
    (
        tokens,
        norm_gains,
        gate_weight,
        value_weight,
        gate_scale,
        value_scale,
        conv_gate,
        conv_value,
        down_weight,
        down_scale,
    ) = args
    if not fits(ra_count, cb_count, tokens, gate_weight, conv_gate):
        return on_device(*args)
    f32, bf16 = jnp.float32, jnp.bfloat16
    layers, width, units = gate_weight.shape
    groups, rows = tokens.shape[0] // GROUP, GROUP
    x_count = cb_count // CORES
    chunk_cols = x_count * LANES
    pairs = pl.cdiv(units // chunk_cols, CORES)
    z_block = rows // ra_count
    parts, events = layers * groups, (layers + 1) * groups
    vmem, dma = pltpu.VMEM, pltpu.SemaphoreType.DMA
    in_vmem, in_hbm = pl.BlockSpec(memory_space=pltpu.VMEM), pl.BlockSpec(memory_space=pl.ANY)
    result = pl.pallas_call(
        functools.partial(fused_kernel, ra_count, cb_count),
        out_shape=jax.ShapeDtypeStruct((groups, rows, width), bf16),
        in_specs=[in_vmem, in_vmem, in_hbm, in_hbm] + [in_vmem] * 4 + [in_hbm, in_vmem],
        out_specs=in_vmem,
        scratch_shapes=[
            vmem((WIDE_SLOTS, width, 2 * chunk_cols), f32),
            vmem((DOWN_SLOTS, chunk_cols, width), f32),
            vmem((layers + 1, groups, ra_count, z_block, width), bf16),
            vmem((groups, rows, width), f32),
            vmem((groups, rows, LANES), f32),
            vmem((rows + 8, 2 * LANES), f32),
            vmem((pairs, 8, 2 * LANES), f32),
            vmem((RING, x_count, rows, 2 * LANES), bf16),
            vmem((RING, x_count, rows, 2 * LANES), bf16),
            vmem((RING, x_count, rows, 2 * LANES), f32),
            vmem((RING, x_count, rows, 2 * LANES), bf16),
            vmem((RING, x_count, rows, 2 * LANES), bf16),
            vmem((RING, cb_count, rows, LANES), bf16),
            vmem((rows, width), f32),
            vmem((parts, ra_count, z_block, width), bf16),
            vmem((parts, ra_count, z_block, width), bf16),
            vmem((parts, z_block, width), f32),
            vmem((events, 8, LANES), f32),
            vmem((events, cb_count, 8, LANES), f32),
            dma((WIDE_SLOTS, 2)),
            dma((DOWN_SLOTS,)),
            dma((RING,)),
            dma((RING,)),
            dma((RING, x_count)),
            dma((RING, x_count)),
            dma((RING, x_count)),
            dma((RING, x_count)),
            dma((RING,)),
            dma((RING,)),
            dma((parts, ra_count)),
            dma((parts, ra_count)),
            dma((parts, ra_count)),
            dma((parts, ra_count)),
            dma((events, cb_count)),
            dma((events, cb_count)),
        ],
        compiler_params=pltpu.CompilerParams(
            collective_id=0, has_side_effects=True, vmem_limit_bytes=67043328
        ),
        name="fused_sublayers",
    )(
        tokens.reshape(groups, rows, width),
        norm_gains,
        gate_weight,
        value_weight,
        gate_scale,
        value_scale,
        conv_gate.transpose(1, 0, 2),
        conv_value.transpose(1, 0, 2),
        down_weight,
        down_scale,
    )
    return result.reshape(groups * rows, width)


def solution(mesh):
    in_specs = (
        P("grp", "cb"),
        P(None, "cb"),
        P(None, "cb", "ra"),
        P(None, "cb", "ra"),
        P(None, "ra"),
        P(None, "ra"),
        P(None, None, "ra"),
        P(None, None, "ra"),
        P(None, "ra", "cb"),
        P(None, "cb"),
    )
    out_specs = P("grp", "cb")
    return jax.shard_map(
        functools.partial(on_device_any, mesh.shape["ra"], mesh.shape["cb"]), mesh=mesh, in_specs=in_specs, out_specs=out_specs, check_vma=False
    )
```

```python
import functools

import jax
import jax.numpy as jnp
from jax import lax
from jax.experimental import pallas as pl
from jax.experimental.pallas import tpu as pltpu
from jax.sharding import PartitionSpec as P

epsilon = 1e-06
residual_weight = 0.5


def causal_taps(projected, tap_weights):
    tap_count = tap_weights.shape[0]
    row_count = projected.shape[0]
    padded = jnp.pad(projected, ((tap_count - 1, 0), (0, 0)))
    result = jnp.zeros_like(projected)
    for tap_idx in range(tap_count):
        result = result + padded[tap_idx : tap_idx + row_count] * tap_weights[tap_idx]
    return result


def row_inverse(state_wide, model_width):
    squares = lax.psum(jnp.sum(state_wide * state_wide, axis=1, keepdims=True), "cb")
    return lax.rsqrt(squares / model_width + epsilon)


def on_device(
    tokens,
    norm_gains,
    gate_weight,
    value_weight,
    gate_scale,
    value_scale,
    conv_gate,
    conv_value,
    down_weight,
    down_scale,
):
    model_width = lax.axis_size("cb") * tokens.shape[1]
    layer_count = gate_weight.shape[0]
    current = tokens
    for layer_idx in range(layer_count):
        state_wide = current.astype(jnp.float32)
        inverse = row_inverse(state_wide, model_width)
        scaled = (state_wide * norm_gains[layer_idx]).astype(jnp.bfloat16)
        gate_part = jnp.dot(
            scaled, gate_weight[layer_idx].astype(jnp.bfloat16), preferred_element_type=jnp.float32
        )
        value_part = jnp.dot(
            scaled, value_weight[layer_idx].astype(jnp.bfloat16), preferred_element_type=jnp.float32
        )
        gate_sum, value_sum = (
            lax.psum_scatter(gate_part, "cb", scatter_dimension=1, tiled=True),
            lax.psum_scatter(value_part, "cb", scatter_dimension=1, tiled=True),
        )
        share_cols = gate_sum.shape[1]
        first_col = lax.axis_index("cb") * share_cols
        gate_cols = lax.dynamic_slice_in_dim(gate_scale[layer_idx], first_col, share_cols, 0)
        value_cols = lax.dynamic_slice_in_dim(value_scale[layer_idx], first_col, share_cols, 0)
        gate_taps = lax.dynamic_slice_in_dim(conv_gate[layer_idx], first_col, share_cols, 1)
        value_taps = lax.dynamic_slice_in_dim(conv_value[layer_idx], first_col, share_cols, 1)
        gate_pre = inverse * gate_cols * gate_sum
        value_pre = inverse * value_cols * value_sum
        hidden = (
            jax.nn.gelu(causal_taps(gate_pre, gate_taps), approximate=True)
            * causal_taps(value_pre, value_taps)
        ).astype(jnp.bfloat16)
        hidden = lax.all_gather(hidden, "cb", axis=1, tiled=True)
        partial_value = jnp.dot(
            hidden, down_weight[layer_idx].astype(jnp.bfloat16), preferred_element_type=jnp.float32
        )
        down_total = lax.psum(partial_value, "ra")
        current = (residual_weight * state_wide + down_scale[layer_idx] * down_total).astype(
            jnp.bfloat16
        )
    state_wide = current.astype(jnp.float32)
    inverse = row_inverse(state_wide, model_width)
    return (state_wide * inverse * norm_gains[layer_count]).astype(jnp.bfloat16)


CORES = 2
LANES = 128
GROUP = 64
RING = 12
WIDE_SLOTS = 16
DOWN_SLOTS = 16
FIRST_LOADS = 6
DOWN_LAG = 3
BUBBLES = 2
PAIR_SUM, GATED, PAIR_GATHER, DOWN = 1, 5, 8, 9
Z_SUM, Z_GATHER = 5, 12
LAST_SUM, LAST_SQUARES, LAST_GATHER = 9, 13, 22


def fused_kernel(
    ra_count,
    cb_count,
    tokens_hbm,
    gains_hbm,
    gate_hbm,
    value_hbm,
    gate_scale_hbm,
    value_scale_hbm,
    conv_gate_hbm,
    conv_value_hbm,
    down_hbm,
    down_scale_hbm,
    out_hbm,
    gains,
    gate_scale,
    value_scale,
    conv_gate,
    conv_value,
    down_scale,
    out,
    wide_weight,
    down_weight,
    current,
    scaled,
    inverse,
    padded,
    carry,
    pair_send,
    pair_recv,
    pair_own,
    x_send,
    x_recv,
    hidden,
    acc,
    z_send,
    z_recv,
    z_own,
    sq_send,
    sq_recv,
    last_send,
    last_recv,
    block_recv,
    small_sem,
    out_sem,
    wide_sem,
    down_sem,
    pair_ss,
    pair_rs,
    x_ss,
    x_rs,
    hx_ss,
    hx_rs,
    hp_ss,
    hp_rs,
    z_ss,
    z_rs,
    c_ss,
    c_rs,
    sq_ss,
    sq_rs,
    last_ss,
    last_rs,
    block_ss,
    block_rs,
):
    f32, bf16 = jnp.float32, jnp.bfloat16
    layers = gate_hbm.shape[0]
    groups, _, z_block, width = tokens_hbm.shape
    rows = ra_count * z_block
    x_count = cb_count // CORES
    chunk_cols = x_count * LANES
    chunks = gate_hbm.shape[2] // chunk_cols
    pairs = pl.cdiv(chunks, CORES)
    taps = conv_gate.shape[0]
    model_width = width * cb_count
    per_layer = groups * pairs
    period = per_layer + BUBBLES
    last_item = layers * period - BUBBLES
    all_groups = groups + (BUBBLES > 0)
    streamed = layers * chunks

    me_cb = lax.axis_index("cb")
    me_ra = lax.axis_index("ra")
    me_x, me_core = lax.div(me_cb, CORES), lax.rem(me_cb, CORES)
    partner = me_x * CORES + (1 - me_core)

    def others(count, me):
        return [lax.rem(me + step, count) for step in range(1, count)]

    def remote(src, dst, send, recv, axis, index):
        return pltpu.make_async_remote_copy(
            src_ref=src,
            dst_ref=dst,
            send_sem=send,
            recv_sem=recv,
            device_id={axis: index},
            device_id_type=pl.DeviceIdType.MESH,
        )

    cb_peers, ra_peers, x_peers = others(cb_count, me_cb), others(ra_count, me_ra), others(x_count, me_x)

    def cb_of(x_index):
        return x_index * CORES + me_core

    def place_of(n):
        layer = sum((jnp.asarray(n >= later * chunks).astype(jnp.int32) for later in range(1, layers)), 0)
        return layer, n - layer * chunks

    def wide_copies(n):
        (layer, chunk), slot = place_of(n), lax.rem(n, WIDE_SLOTS)
        cols = pl.ds(pl.multiple_of(chunk * chunk_cols, chunk_cols), chunk_cols)
        return (
            pltpu.make_async_copy(
                gate_hbm.at[layer, :, cols],
                wide_weight.at[slot, :, pl.ds(0, chunk_cols)],
                wide_sem.at[slot, 0],
            ),
            pltpu.make_async_copy(
                value_hbm.at[layer, :, cols],
                wide_weight.at[slot, :, pl.ds(chunk_cols, chunk_cols)],
                wide_sem.at[slot, 1],
            ),
        )

    def down_copies(n):
        (layer, chunk), slot = place_of(n), lax.rem(n, DOWN_SLOTS)
        cols = pl.ds(pl.multiple_of(chunk * chunk_cols, chunk_cols), chunk_cols)
        return (
            pltpu.make_async_copy(down_hbm.at[layer, cols, :], down_weight.at[slot], down_sem.at[slot]),
        )

    def start_copies(copies, n, limit):
        @pl.when(n < limit)
        def _():
            for copy in copies(n):
                copy.start()

    barrier = pltpu.get_barrier_semaphore()
    for axis, peers in (("cb", cb_peers), ("ra", ra_peers)):
        for peer in peers:
            pl.semaphore_signal(
                barrier, inc=1, device_id={axis: peer}, device_id_type=pl.DeviceIdType.MESH
            )

    small = [
        pltpu.make_async_copy(source, place, small_sem.at[n])
        for n, (source, place) in enumerate(
            (
                (tokens_hbm, current.at[0]),
                (gains_hbm, gains),
                (gate_scale_hbm, gate_scale),
                (value_scale_hbm, value_scale),
                (conv_gate_hbm, conv_gate),
                (conv_value_hbm, conv_value),
                (down_scale_hbm, down_scale),
            )
        )
    ]
    for copy in small[:2]:
        copy.start()
    for n in range(min(FIRST_LOADS, streamed)):
        for copy in wide_copies(n):
            copy.start()
    for copy in small[2:]:
        copy.start()

    def pair_copy(slot):
        return remote(
            pair_send.at[slot], pair_recv.at[slot], pair_ss.at[slot], pair_rs.at[slot], "cb", partner
        )

    def x_copy(slot, peer, source):
        return remote(
            x_send.at[slot, peer],
            x_recv.at[slot, source],
            x_ss.at[slot, peer],
            x_rs.at[slot, source],
            "cb",
            cb_of(peer),
        )

    def hx_copy(slot, peer, source):
        place = hidden.at[slot, me_core * x_count + source]
        return remote(place, place, hx_ss.at[slot, peer], hx_rs.at[slot, source], "cb", cb_of(peer))

    def hp_copy(slot, core):
        place = hidden.at[slot, pl.ds(core * x_count, x_count)]
        return remote(place, place, hp_ss.at[slot], hp_rs.at[slot], "cb", partner)

    def z_copy(part, peer, source):
        return remote(
            z_send.at[part, peer],
            z_recv.at[part, source],
            z_ss.at[part, peer],
            z_rs.at[part, source],
            "ra",
            peer,
        )

    def c_copy(part, layer, group, peer, source):
        place = current.at[layer, group, source]
        return remote(place, place, c_ss.at[part, peer], c_rs.at[part, source], "ra", peer)

    def sq_copy(event, peer, source):
        return remote(
            sq_send.at[event], sq_recv.at[event, source], sq_ss.at[event, peer], sq_rs.at[event, source], "cb", peer
        )

    def scale_rows(layer, group):
        event = layer * groups + group
        wide = current[layer, group].reshape(rows, width).astype(f32)
        scaled[group] = (wide * gains[pl.ds(layer, 1), :]).astype(bf16).astype(f32)
        squares = jnp.broadcast_to(jnp.sum(wide * wide, axis=1, keepdims=True), (rows, LANES))
        sq_send[event] = jnp.concatenate([squares] * (LANES // rows), axis=0).T[:8]

    def send_squares(layer, group):
        for peer in cb_peers:
            sq_copy(layer * groups + group, peer, me_cb).start()

    def finish_squares(layer, group):
        event = layer * groups + group
        total = sq_send[event]
        for peer in cb_peers:
            copy = sq_copy(event, peer, peer)
            copy.wait_send()
            copy.wait_recv()
            total = total + sq_recv[event, peer]
        row = lax.rsqrt(total / model_width + epsilon)
        inverse[group] = jnp.broadcast_to(row[:1], (LANES, LANES)).T[:rows]

    for copy in small[:2]:
        copy.wait()
    for group in range(groups):
        scale_rows(0, group)
    pl.semaphore_wait(barrier, cb_count + ra_count - 2)
    for group in range(groups):
        send_squares(0, group)
    for copy in small[2:]:
        copy.wait()

    def when_full(pair, both, first_only):
        if chunks % CORES == 0:
            both()
        else:
            pl.when(pair < pairs - 1)(both)
            pl.when(pair == pairs - 1)(first_only)

    def when_owner(pair, fn):
        if chunks % CORES == 0:
            fn()
        else:
            pl.when((pair < pairs - 1) | (me_core == 0))(fn)

    def when_partner(pair, fn):
        if chunks % CORES == 0:
            fn()
        else:
            pl.when((pair < pairs - 1) | (me_core == 1))(fn)

    def project_ready(layer, group, pair, slot):
        ordinal = group * pairs + pair
        first = layer * chunks + pair * CORES
        end = (layer + 1) * chunks

        @pl.when(layer == 0)
        def _():
            for n in range(CORES):
                start_copies(wide_copies, FIRST_LOADS + ordinal * CORES + n, min(WIDE_SLOTS, streamed))

            @pl.when(ordinal >= DOWN_LAG)
            def _():
                for n in range(CORES):
                    start_copies(down_copies, (ordinal - DOWN_LAG) * CORES + n, min(DOWN_SLOTS, streamed))

        @pl.when(group == 0)
        def _():
            for n in range(CORES):

                @pl.when(first + n < end)
                def _(n=n):
                    for copy in wide_copies(first + n):
                        copy.wait()

    def project_parts(layer, group, pair, slot):
        first = layer * chunks + pair * CORES

        def product_of(chunk_at):
            return jnp.dot(
                scaled[group], wide_weight[lax.rem(chunk_at, WIDE_SLOTS)], preferred_element_type=f32
            )

        def keep(chunk_at):
            product = product_of(chunk_at)
            for x in range(x_count):
                for kind in range(2):
                    at = kind * chunk_cols + x * LANES
                    pair_own[slot, x, :, kind * LANES : (kind + 1) * LANES] = product[:, at : at + LANES]

        def give(chunk_at):
            product = product_of(chunk_at)
            for x in range(x_count):
                for kind in range(2):
                    at = kind * chunk_cols + x * LANES
                    pair_send[slot, x, :, kind * LANES : (kind + 1) * LANES] = product[
                        :, at : at + LANES
                    ].astype(bf16)

        def both():
            give(first + 1 - me_core)
            pair_copy(slot).start()
            keep(first + me_core)

        def first_only():
            @pl.when(me_core == 0)
            def _():
                keep(first)

            @pl.when(me_core == 1)
            def _():
                give(first)
                pair_copy(slot).start()

        return both, first_only

    def project_done(layer, group, pair, slot):
        first = layer * chunks + pair * CORES
        end = (layer + 1) * chunks

        @pl.when(group == groups - 1)
        def _():
            for n in range(CORES):

                @pl.when(first + n < end)
                def _(n=n):
                    start_copies(wide_copies, first + n + WIDE_SLOTS, streamed)

    def pair_sum(layer, group, pair, slot):
        when_partner(pair, lambda: pair_copy(slot).wait_send())

        def send():
            pair_copy(slot).wait_recv()
            for peer in x_peers:
                x_send[slot, peer] = (pair_own[slot, peer] + pair_recv[slot, peer].astype(f32)).astype(bf16)
                x_copy(slot, peer, me_x).start()

        when_owner(pair, send)

    def gated(layer, group, pair, slot):
        @pl.when(pair == 0)
        def _():
            finish_squares(layer, group)

        def unit():
            total = pair_own[slot, me_x] + pair_recv[slot, me_x].astype(f32)
            for peer in x_peers:
                copy = x_copy(slot, peer, peer)
                copy.wait_send()
                copy.wait_recv()
                total = total + x_recv[slot, peer].astype(f32)
            at = (pair * CORES + me_core) * chunk_cols
            cols = pl.ds(pl.multiple_of(at, chunk_cols), chunk_cols)
            one = pl.ds(layer, 1)

            def mine(values):
                kept = values[:, :LANES]
                for x in range(1, x_count):
                    kept = jnp.where(me_x == x, values[:, x * LANES : (x + 1) * LANES], kept)
                return kept

            scales = jnp.concatenate([mine(gate_scale[one, cols]), mine(value_scale[one, cols])], axis=1)
            weights = jnp.concatenate(
                [mine(conv_gate[:, layer, cols]), mine(conv_value[:, layer, cols])], axis=1
            )
            inv = inverse[group]
            pre = total * jnp.concatenate([inv, inv], axis=1) * scales
            before = carry[pair]
            padded[:8] = jnp.where(group == 0, jnp.zeros_like(before), before)
            padded[8:] = pre
            carry[pair] = pre[rows - 8 :]
            mixed = pre * weights[taps - 1 : taps]
            for tap in range(taps - 1):
                mixed = mixed + padded[pl.ds(8 - (taps - 1) + tap, rows), :] * weights[tap : tap + 1]
            hidden[slot, me_core * x_count + me_x] = (
                jax.nn.gelu(mixed[:, :LANES], approximate=True) * mixed[:, LANES:]
            ).astype(bf16)
            for peer in x_peers:
                hx_copy(slot, peer, me_x).start()

        when_owner(pair, unit)

    def pair_gather(layer, group, pair, slot):
        def forward():
            for peer in x_peers:
                hx_copy(slot, peer, me_x).wait_send()
                hx_copy(slot, peer, peer).wait_recv()
            hp_copy(slot, me_core).start()

        when_owner(pair, forward)

    def down_ready(layer, group, pair, slot):
        first = layer * chunks + pair * CORES
        end = (layer + 1) * chunks

        @pl.when(group == 0)
        def _():
            for n in range(CORES):

                @pl.when(first + n < end)
                def _(n=n):
                    for copy in down_copies(first + n):
                        copy.wait()

        when_owner(pair, lambda: hp_copy(slot, me_core).wait_send())
        when_partner(pair, lambda: hp_copy(slot, 1 - me_core).wait_recv())

    def down_parts(layer, group, pair, slot):
        first = layer * chunks + pair * CORES

        def add(count):
            left = jnp.concatenate([hidden[slot, n] for n in range(count * x_count)], axis=1).astype(f32)
            right = jnp.concatenate(
                [down_weight[lax.rem(first + n, DOWN_SLOTS)] for n in range(count)], axis=0
            )
            product = jnp.dot(left, right, preferred_element_type=f32)
            before = acc[...]
            acc[...] = jnp.where(pair == 0, jnp.zeros_like(before), before) + product

        return lambda: add(CORES), lambda: add(1)

    def down_done(layer, group, pair, slot):
        first = layer * chunks + pair * CORES
        end = (layer + 1) * chunks

        @pl.when(group == groups - 1)
        def _():
            for n in range(CORES):

                @pl.when(first + n < end)
                def _(n=n):
                    start_copies(down_copies, first + n + DOWN_SLOTS, streamed)

        @pl.when(pair == pairs - 1)
        def _():
            part = layer * groups + group
            total = acc[...].reshape(ra_count, z_block, width)
            z_send[part] = total.astype(bf16)
            z_own[part] = acc[pl.ds(pl.multiple_of(me_ra * z_block, z_block), z_block), :]
            for peer in ra_peers:
                z_copy(part, peer, me_ra).start()

    def z_sum(layer, group, pair, slot):
        part = layer * groups + group
        total = z_own[part]
        for peer in ra_peers:
            copy = z_copy(part, peer, peer)
            copy.wait_send()
            copy.wait_recv()
            total = total + z_recv[part, peer].astype(f32)
        kept = residual_weight * current[layer, group, me_ra].astype(f32)
        block = (kept + down_scale[pl.ds(layer, 1), :] * total).astype(bf16)
        current[layer + 1, group, me_ra] = block
        for peer in ra_peers:
            c_copy(part, layer + 1, group, peer, me_ra).start()
        return block

    def last_sum(layer, group, pair, slot):
        wide = z_sum(layer, group, pair, slot).astype(f32)
        squares = jnp.broadcast_to(jnp.sum(wide * wide, axis=1, keepdims=True), (z_block, LANES))
        last_send[group] = jnp.concatenate([squares] * (LANES // z_block), axis=0).T[:8]
        for peer in cb_peers:
            last_copy(group, peer, me_cb).start()

    def last_squares(layer, group, pair, slot):
        total = last_send[group]
        for peer in cb_peers:
            copy = last_copy(group, peer, peer)
            copy.wait_send()
            copy.wait_recv()
            total = total + last_recv[group, peer]
        block_recv[group, me_ra] = total
        for peer in ra_peers:
            block_copy(group, peer, me_ra).start()

    def wait_blocks(layer, group):
        part = layer * groups + group
        for peer in ra_peers:
            c_copy(part, layer + 1, group, peer, me_ra).wait_send()
            c_copy(part, layer + 1, group, peer, peer).wait_recv()

    def z_gather(layer, group, pair, slot):
        wait_blocks(layer, group)
        scale_rows(layer + 1, group)
        send_squares(layer + 1, group)

    def last_gather(layer, group, pair, slot):
        wait_blocks(layer, group)
        for peer in ra_peers:
            block_copy(group, peer, me_ra).wait_send()
            block_copy(group, peer, peer).wait_recv()
        lane = lax.broadcasted_iota(jnp.int32, (8, LANES), 1)
        squares = jnp.zeros((8, LANES), f32)
        for ra_at in range(ra_count):
            inside = (lane >= ra_at * z_block) & (lane < (ra_at + 1) * z_block)
            squares = jnp.where(inside, block_recv[group, ra_at], squares)
        row = lax.rsqrt(squares / model_width + epsilon)
        inv = jnp.broadcast_to(row[:1], (LANES, LANES)).T[:rows]
        wide = current[layers, group].reshape(rows, width).astype(f32)
        inv = jnp.concatenate([inv] * (width // LANES), axis=1)
        out[group] = (wide * inv * gains[pl.ds(layers, 1), :]).astype(bf16)
        out_copy(group).start()

    def out_copy(group):
        return pltpu.make_async_copy(out.at[group], out_hbm.at[group], out_sem.at[group])

    def last_copy(group, peer, source):
        return remote(
            last_send.at[group], last_recv.at[group, source], last_ss.at[group, peer], last_rs.at[group, source], "cb", peer
        )

    def block_copy(group, peer, source):
        place = block_recv.at[group, source]
        return remote(place, place, block_ss.at[group, peer], block_rs.at[group, source], "ra", peer)

    stages = (
        (DOWN + LAST_GATHER, "last", last_gather),
        (DOWN + LAST_SQUARES, "last", last_squares),
        (DOWN + LAST_SUM, "last", last_sum),
        (DOWN + Z_GATHER, "inner", z_gather),
        (DOWN + Z_SUM, "inner", z_sum),
        (PAIR_GATHER, "", pair_gather),
        (GATED, "", gated),
    )
    late_stages = ((PAIR_SUM, "", pair_sum),)

    delays = sorted({delay for delay, _, _ in stages + late_stages} | {0, DOWN})

    def started(delay):
        layer, rest = divmod(-delay, period)
        group, pair = (groups, rest - per_layer) if rest >= per_layer else divmod(rest, pairs)
        return tuple(jnp.int32(value) for value in (layer, group, pair, 0))

    def advanced(place):
        layer, group, pair, slot = place
        used = (layer >= 0) & (group < groups)
        slot = jnp.where(used, jnp.where(slot == RING - 1, 0, slot + 1), slot)
        wrap = pair + 1 == jnp.where(group == groups, BUBBLES, pairs)
        pair = jnp.where(wrap, 0, pair + 1)
        group = jnp.where(wrap, group + 1, group)
        next_layer = group == all_groups
        return jnp.where(next_layer, layer + 1, layer), jnp.where(next_layer, 0, group), pair, slot

    def multiply(wide_place, down_place):
        def valid(place):
            return (place[0] >= 0) & (place[0] < layers) & (place[1] < groups)

        def full(place):
            return place[2] < pairs - chunks % CORES

        wide_on, down_on = valid(wide_place), valid(down_place)
        merged = wide_on & down_on & full(wide_place) & full(down_place)
        pl.when(wide_on)(lambda: project_ready(*wide_place))
        pl.when(down_on)(lambda: down_ready(*down_place))

        @pl.when(merged)
        def _():
            project_parts(*wide_place)[0]()
            down_parts(*down_place)[0]()

        @pl.when(wide_on & jnp.logical_not(merged))
        def _():
            when_full(wide_place[2], *project_parts(*wide_place))

        @pl.when(down_on & jnp.logical_not(merged))
        def _():
            when_full(down_place[2], *down_parts(*down_place))

        pl.when(wide_on)(lambda: project_done(*wide_place))
        pl.when(down_on)(lambda: down_done(*down_place))

    def step(index, places):
        run_stages(stages, places)
        multiply(places[delays.index(0)], places[delays.index(DOWN)])
        run_stages(late_stages, places)
        return tuple(advanced(place) for place in places)

    def run_stages(chosen, places):
        for delay, ending, stage in chosen:
            place = places[delays.index(delay)]
            layer, group, pair, slot = place
            valid = (layer >= 0) & (layer < layers) & (group < groups)
            if ending:
                valid = valid & (pair == pairs - 1) & ((layer == layers - 1) == (ending == "last"))

            @pl.when(valid)
            def _(stage=stage, place=place):
                stage(*place)

    lax.fori_loop(0, last_item + DOWN + LAST_GATHER, step, tuple(started(delay) for delay in delays))
    for group in range(groups):
        out_copy(group).wait()


def fits(ra_count, cb_count, tokens, gate_weight, conv_gate):
    rows, width = tokens.shape
    layers, _, units = gate_weight.shape
    if cb_count % CORES or cb_count <= CORES or ra_count < 2 or rows % GROUP or GROUP % (16 * ra_count):
        return False
    chunk_cols = cb_count // CORES * LANES
    if width % LANES or units % chunk_cols or units // chunk_cols < CORES or conv_gate.shape[1] > 9:
        return False
    chunks = units // chunk_cols
    pairs, groups = pl.cdiv(chunks, CORES), rows // GROUP
    weights = 4 * width * chunk_cols * (2 * WIDE_SLOTS + DOWN_SLOTS)
    return (
        chunks <= min(WIDE_SLOTS, DOWN_SLOTS)
        and (groups - 1) * pairs + 1 + BUBBLES >= DOWN + Z_GATHER
        and weights + 4 * rows * width * 12 <= 60 * 1024 * 1024
    )


def on_device_any(ra_count, cb_count, *args):
    (
        tokens,
        norm_gains,
        gate_weight,
        value_weight,
        gate_scale,
        value_scale,
        conv_gate,
        conv_value,
        down_weight,
        down_scale,
    ) = args
    if not fits(ra_count, cb_count, tokens, gate_weight, conv_gate):
        return on_device(*args)
    f32, bf16 = jnp.float32, jnp.bfloat16
    layers, width, units = gate_weight.shape
    groups, rows = tokens.shape[0] // GROUP, GROUP
    x_count = cb_count // CORES
    chunk_cols = x_count * LANES
    pairs = pl.cdiv(units // chunk_cols, CORES)
    z_block = rows // ra_count
    parts, events = layers * groups, layers * groups
    vmem, dma = pltpu.VMEM, pltpu.SemaphoreType.DMA
    in_hbm = pl.BlockSpec(memory_space=pl.ANY)
    taps = conv_gate.shape[1]
    result = pl.pallas_call(
        functools.partial(fused_kernel, ra_count, cb_count),
        out_shape=jax.ShapeDtypeStruct((groups, rows, width), bf16),
        in_specs=[in_hbm] * 10,
        out_specs=in_hbm,
        scratch_shapes=[
            vmem(norm_gains.shape, f32),
            vmem(gate_scale.shape, f32),
            vmem(value_scale.shape, f32),
            vmem((taps, layers, units), f32),
            vmem((taps, layers, units), f32),
            vmem(down_scale.shape, f32),
            vmem((groups, rows, width), bf16),
            vmem((WIDE_SLOTS, width, 2 * chunk_cols), f32),
            vmem((DOWN_SLOTS, chunk_cols, width), f32),
            vmem((layers + 1, groups, ra_count, z_block, width), bf16),
            vmem((groups, rows, width), f32),
            vmem((groups, rows, LANES), f32),
            vmem((rows + 8, 2 * LANES), f32),
            vmem((pairs, 8, 2 * LANES), f32),
            vmem((RING, x_count, rows, 2 * LANES), bf16),
            vmem((RING, x_count, rows, 2 * LANES), bf16),
            vmem((RING, x_count, rows, 2 * LANES), f32),
            vmem((RING, x_count, rows, 2 * LANES), bf16),
            vmem((RING, x_count, rows, 2 * LANES), bf16),
            vmem((RING, cb_count, rows, LANES), bf16),
            vmem((rows, width), f32),
            vmem((parts, ra_count, z_block, width), bf16),
            vmem((parts, ra_count, z_block, width), bf16),
            vmem((parts, z_block, width), f32),
            vmem((events, 8, LANES), f32),
            vmem((events, cb_count, 8, LANES), f32),
            vmem((groups, 8, LANES), f32),
            vmem((groups, cb_count, 8, LANES), f32),
            vmem((groups, ra_count, 8, LANES), f32),
            dma((7,)),
            dma((groups,)),
            dma((WIDE_SLOTS, 2)),
            dma((DOWN_SLOTS,)),
            dma((RING,)),
            dma((RING,)),
            dma((RING, x_count)),
            dma((RING, x_count)),
            dma((RING, x_count)),
            dma((RING, x_count)),
            dma((RING,)),
            dma((RING,)),
            dma((parts, ra_count)),
            dma((parts, ra_count)),
            dma((parts, ra_count)),
            dma((parts, ra_count)),
            dma((events, cb_count)),
            dma((events, cb_count)),
            dma((groups, cb_count)),
            dma((groups, cb_count)),
            dma((groups, ra_count)),
            dma((groups, ra_count)),
        ],
        compiler_params=pltpu.CompilerParams(
            collective_id=0, has_side_effects=True, vmem_limit_bytes=67043328
        ),
        name="fused_sublayers",
    )(
        tokens.reshape(groups, ra_count, z_block, width),
        norm_gains,
        gate_weight,
        value_weight,
        gate_scale,
        value_scale,
        conv_gate.transpose(1, 0, 2),
        conv_value.transpose(1, 0, 2),
        down_weight,
        down_scale,
    )
    return result.reshape(groups * rows, width)


def solution(mesh):
    in_specs = (
        P("grp", "cb"),
        P(None, "cb"),
        P(None, "cb", "ra"),
        P(None, "cb", "ra"),
        P(None, "ra"),
        P(None, "ra"),
        P(None, None, "ra"),
        P(None, None, "ra"),
        P(None, "ra", "cb"),
        P(None, "cb"),
    )
    out_specs = P("grp", "cb")
    return jax.shard_map(
        functools.partial(on_device_any, mesh.shape["ra"], mesh.shape["cb"]), mesh=mesh, in_specs=in_specs, out_specs=out_specs, check_vma=False
    )
```

```python
import functools

import jax
import jax.numpy as jnp
from jax import lax
from jax.experimental import pallas as pl
from jax.experimental.pallas import tpu as pltpu
from jax.sharding import PartitionSpec as P

epsilon = 1e-06
residual_weight = 0.5


def causal_taps(projected, tap_weights):
    tap_count = tap_weights.shape[0]
    row_count = projected.shape[0]
    padded = jnp.pad(projected, ((tap_count - 1, 0), (0, 0)))
    result = jnp.zeros_like(projected)
    for tap_idx in range(tap_count):
        result = result + padded[tap_idx : tap_idx + row_count] * tap_weights[tap_idx]
    return result


def row_inverse(state_wide, model_width):
    squares = lax.psum(jnp.sum(state_wide * state_wide, axis=1, keepdims=True), "cb")
    return lax.rsqrt(squares / model_width + epsilon)


def on_device(
    tokens,
    norm_gains,
    gate_weight,
    value_weight,
    gate_scale,
    value_scale,
    conv_gate,
    conv_value,
    down_weight,
    down_scale,
):
    model_width = lax.axis_size("cb") * tokens.shape[1]
    layer_count = gate_weight.shape[0]
    current = tokens
    for layer_idx in range(layer_count):
        state_wide = current.astype(jnp.float32)
        inverse = row_inverse(state_wide, model_width)
        scaled = (state_wide * norm_gains[layer_idx]).astype(jnp.bfloat16)
        gate_part = jnp.dot(
            scaled, gate_weight[layer_idx].astype(jnp.bfloat16), preferred_element_type=jnp.float32
        )
        value_part = jnp.dot(
            scaled, value_weight[layer_idx].astype(jnp.bfloat16), preferred_element_type=jnp.float32
        )
        gate_sum, value_sum = (
            lax.psum_scatter(gate_part, "cb", scatter_dimension=1, tiled=True),
            lax.psum_scatter(value_part, "cb", scatter_dimension=1, tiled=True),
        )
        share_cols = gate_sum.shape[1]
        first_col = lax.axis_index("cb") * share_cols
        gate_cols = lax.dynamic_slice_in_dim(gate_scale[layer_idx], first_col, share_cols, 0)
        value_cols = lax.dynamic_slice_in_dim(value_scale[layer_idx], first_col, share_cols, 0)
        gate_taps = lax.dynamic_slice_in_dim(conv_gate[layer_idx], first_col, share_cols, 1)
        value_taps = lax.dynamic_slice_in_dim(conv_value[layer_idx], first_col, share_cols, 1)
        gate_pre = inverse * gate_cols * gate_sum
        value_pre = inverse * value_cols * value_sum
        hidden = (
            jax.nn.gelu(causal_taps(gate_pre, gate_taps), approximate=True)
            * causal_taps(value_pre, value_taps)
        ).astype(jnp.bfloat16)
        hidden = lax.all_gather(hidden, "cb", axis=1, tiled=True)
        partial_value = jnp.dot(
            hidden, down_weight[layer_idx].astype(jnp.bfloat16), preferred_element_type=jnp.float32
        )
        down_total = lax.psum(partial_value, "ra")
        current = (residual_weight * state_wide + down_scale[layer_idx] * down_total).astype(
            jnp.bfloat16
        )
    state_wide = current.astype(jnp.float32)
    inverse = row_inverse(state_wide, model_width)
    return (state_wide * inverse * norm_gains[layer_count]).astype(jnp.bfloat16)


CORES = 2
LANES = 128
GROUP = 64
RING = 12
WIDE_SLOTS = 16
DOWN_SLOTS = 16
FIRST_LOADS = 6
DOWN_LAG = 3
BUBBLES = 2
PAIR_SUM, GATED, PAIR_GATHER, DOWN = 1, 5, 8, 9
Z_SUM, Z_GATHER = 5, 12
LAST_SUM, LAST_SQUARES, LAST_GATHER = 9, 13, 22


def fused_kernel(
    ra_count,
    cb_count,
    tokens_hbm,
    gains_hbm,
    gate_hbm,
    value_hbm,
    gate_scale_hbm,
    value_scale_hbm,
    conv_gate_hbm,
    conv_value_hbm,
    down_hbm,
    down_scale_hbm,
    out_hbm,
    gains,
    gate_scale,
    value_scale,
    conv_gate,
    conv_value,
    down_scale,
    out,
    wide_weight,
    down_weight,
    current,
    scaled,
    inverse,
    padded,
    carry,
    pair_send,
    pair_recv,
    pair_own,
    x_send,
    x_recv,
    hidden,
    acc,
    z_send,
    z_recv,
    z_own,
    sq_send,
    sq_recv,
    last_send,
    last_recv,
    block_recv,
    small_sem,
    out_sem,
    wide_sem,
    down_sem,
    pair_ss,
    pair_rs,
    x_ss,
    x_rs,
    hx_ss,
    hx_rs,
    hp_ss,
    hp_rs,
    z_ss,
    z_rs,
    c_ss,
    c_rs,
    sq_ss,
    sq_rs,
    last_ss,
    last_rs,
    block_ss,
    block_rs,
):
    f32, bf16 = jnp.float32, jnp.bfloat16
    layers = gate_hbm.shape[0]
    groups, _, z_block, width = tokens_hbm.shape
    rows = ra_count * z_block
    x_count = cb_count // CORES
    chunk_cols = x_count * LANES
    chunks = gate_hbm.shape[2] // chunk_cols
    pairs = pl.cdiv(chunks, CORES)
    taps = conv_gate.shape[0]
    model_width = width * cb_count
    per_layer = groups * pairs
    period = per_layer + BUBBLES
    last_item = layers * period - BUBBLES
    all_groups = groups + (BUBBLES > 0)
    streamed = layers * chunks

    me_cb = lax.axis_index("cb")
    me_ra = lax.axis_index("ra")
    me_x, me_core = lax.div(me_cb, CORES), lax.rem(me_cb, CORES)
    partner = me_x * CORES + (1 - me_core)

    def others(count, me):
        return [lax.rem(me + step, count) for step in range(1, count)]

    def remote(src, dst, send, recv, axis, index):
        return pltpu.make_async_remote_copy(
            src_ref=src,
            dst_ref=dst,
            send_sem=send,
            recv_sem=recv,
            device_id={axis: index},
            device_id_type=pl.DeviceIdType.MESH,
        )

    def far_first(count, me):
        low = [jnp.where(n >= me, n + 1, n) for n in range(count - 1)]
        high = [jnp.where(count - 1 - n <= me, count - 2 - n, count - 1 - n) for n in range(count - 1)]
        return [jnp.where(2 * me < count, up, down) for up, down in zip(high, low)]

    cb_peers, ra_peers, x_peers = others(cb_count, me_cb), far_first(ra_count, me_ra), others(x_count, me_x)

    def cb_of(x_index):
        return x_index * CORES + me_core

    def place_of(n):
        layer = sum((jnp.asarray(n >= later * chunks).astype(jnp.int32) for later in range(1, layers)), 0)
        return layer, n - layer * chunks

    def wide_copies(n):
        (layer, chunk), slot = place_of(n), lax.rem(n, WIDE_SLOTS)
        cols = pl.ds(pl.multiple_of(chunk * chunk_cols, chunk_cols), chunk_cols)
        return (
            pltpu.make_async_copy(
                gate_hbm.at[layer, :, cols],
                wide_weight.at[slot, :, pl.ds(0, chunk_cols)],
                wide_sem.at[slot, 0],
            ),
            pltpu.make_async_copy(
                value_hbm.at[layer, :, cols],
                wide_weight.at[slot, :, pl.ds(chunk_cols, chunk_cols)],
                wide_sem.at[slot, 1],
            ),
        )

    def down_copies(n):
        (layer, chunk), slot = place_of(n), lax.rem(n, DOWN_SLOTS)
        cols = pl.ds(pl.multiple_of(chunk * chunk_cols, chunk_cols), chunk_cols)
        return (
            pltpu.make_async_copy(down_hbm.at[layer, cols, :], down_weight.at[slot], down_sem.at[slot]),
        )

    def start_copies(copies, n, limit):
        @pl.when(n < limit)
        def _():
            for copy in copies(n):
                copy.start()

    barrier = pltpu.get_barrier_semaphore()
    for axis, peers in (("cb", cb_peers), ("ra", ra_peers)):
        for peer in peers:
            pl.semaphore_signal(
                barrier, inc=1, device_id={axis: peer}, device_id_type=pl.DeviceIdType.MESH
            )

    small = [
        pltpu.make_async_copy(source, place, small_sem.at[n])
        for n, (source, place) in enumerate(
            (
                (tokens_hbm, current.at[0]),
                (gains_hbm, gains),
                (gate_scale_hbm, gate_scale),
                (value_scale_hbm, value_scale),
                (conv_gate_hbm, conv_gate),
                (conv_value_hbm, conv_value),
                (down_scale_hbm, down_scale),
            )
        )
    ]
    for copy in small[:2]:
        copy.start()
    for n in range(min(FIRST_LOADS, streamed)):
        for copy in wide_copies(n):
            copy.start()
    for copy in small[2:]:
        copy.start()

    def pair_copy(slot):
        return remote(
            pair_send.at[slot], pair_recv.at[slot], pair_ss.at[slot], pair_rs.at[slot], "cb", partner
        )

    def x_copy(slot, peer, source):
        return remote(
            x_send.at[slot, peer],
            x_recv.at[slot, source],
            x_ss.at[slot, peer],
            x_rs.at[slot, source],
            "cb",
            cb_of(peer),
        )

    def hx_copy(slot, peer, source):
        place = hidden.at[slot, me_core * x_count + source]
        return remote(place, place, hx_ss.at[slot, peer], hx_rs.at[slot, source], "cb", cb_of(peer))

    def hp_copy(slot, core):
        place = hidden.at[slot, pl.ds(core * x_count, x_count)]
        return remote(place, place, hp_ss.at[slot], hp_rs.at[slot], "cb", partner)

    def z_copy(part, peer, source):
        return remote(
            z_send.at[part, peer],
            z_recv.at[part, source],
            z_ss.at[part, peer],
            z_rs.at[part, source],
            "ra",
            peer,
        )

    def c_copy(part, layer, group, peer, source):
        place = current.at[layer, group, source]
        return remote(place, place, c_ss.at[part, peer], c_rs.at[part, source], "ra", peer)

    def sq_copy(event, peer, source):
        return remote(
            sq_send.at[event], sq_recv.at[event, source], sq_ss.at[event, peer], sq_rs.at[event, source], "cb", peer
        )

    def scale_rows(layer, group):
        event = layer * groups + group
        wide = current[layer, group].reshape(rows, width).astype(f32)
        scaled[group] = (wide * gains[pl.ds(layer, 1), :]).astype(bf16).astype(f32)
        squares = jnp.broadcast_to(jnp.sum(wide * wide, axis=1, keepdims=True), (rows, LANES))
        sq_send[event] = jnp.concatenate([squares] * (LANES // rows), axis=0).T[:8]

    def send_squares(layer, group):
        for peer in cb_peers:
            sq_copy(layer * groups + group, peer, me_cb).start()

    def finish_squares(layer, group):
        event = layer * groups + group
        total = sq_send[event]
        for peer in cb_peers:
            copy = sq_copy(event, peer, peer)
            copy.wait_send()
            copy.wait_recv()
            total = total + sq_recv[event, peer]
        row = lax.rsqrt(total / model_width + epsilon)
        inverse[group] = jnp.broadcast_to(row[:1], (LANES, LANES)).T[:rows]

    for copy in small[:2]:
        copy.wait()
    scale_rows(0, 0)
    pl.semaphore_wait(barrier, cb_count + ra_count - 2)
    send_squares(0, 0)
    for copy in small[2:]:
        copy.wait()

    def when_full(pair, both, first_only):
        if chunks % CORES == 0:
            both()
        else:
            pl.when(pair < pairs - 1)(both)
            pl.when(pair == pairs - 1)(first_only)

    def when_owner(pair, fn):
        if chunks % CORES == 0:
            fn()
        else:
            pl.when((pair < pairs - 1) | (me_core == 0))(fn)

    def when_partner(pair, fn):
        if chunks % CORES == 0:
            fn()
        else:
            pl.when((pair < pairs - 1) | (me_core == 1))(fn)

    def project_ready(layer, group, pair, slot):
        ordinal = group * pairs + pair
        first = layer * chunks + pair * CORES
        end = (layer + 1) * chunks

        @pl.when((layer == 0) & (group > 0) & (pair == 0))
        def _():
            scale_rows(0, group)
            send_squares(0, group)

        @pl.when(layer == 0)
        def _():
            for n in range(CORES):
                start_copies(wide_copies, FIRST_LOADS + ordinal * CORES + n, min(WIDE_SLOTS, streamed))

            @pl.when(ordinal >= DOWN_LAG)
            def _():
                for n in range(CORES):
                    start_copies(down_copies, (ordinal - DOWN_LAG) * CORES + n, min(DOWN_SLOTS, streamed))

        @pl.when(group == 0)
        def _():
            for n in range(CORES):

                @pl.when(first + n < end)
                def _(n=n):
                    for copy in wide_copies(first + n):
                        copy.wait()

    def project_parts(layer, group, pair, slot):
        first = layer * chunks + pair * CORES

        def product_of(chunk_at):
            return jnp.dot(
                scaled[group], wide_weight[lax.rem(chunk_at, WIDE_SLOTS)], preferred_element_type=f32
            )

        def keep(chunk_at):
            product = product_of(chunk_at)
            for x in range(x_count):
                for kind in range(2):
                    at = kind * chunk_cols + x * LANES
                    pair_own[slot, x, :, kind * LANES : (kind + 1) * LANES] = product[:, at : at + LANES]

        def give(chunk_at):
            product = product_of(chunk_at)
            for x in range(x_count):
                for kind in range(2):
                    at = kind * chunk_cols + x * LANES
                    pair_send[slot, x, :, kind * LANES : (kind + 1) * LANES] = product[
                        :, at : at + LANES
                    ].astype(bf16)

        def both():
            give(first + 1 - me_core)
            keep(first + me_core)

        def first_only():
            @pl.when(me_core == 0)
            def _():
                keep(first)

            @pl.when(me_core == 1)
            def _():
                give(first)

        return both, first_only

    def project_done(layer, group, pair, slot):
        first = layer * chunks + pair * CORES
        end = (layer + 1) * chunks

        @pl.when(group == groups - 1)
        def _():
            for n in range(CORES):

                @pl.when(first + n < end)
                def _(n=n):
                    start_copies(wide_copies, first + n + WIDE_SLOTS, streamed)

    def pair_sum(layer, group, pair, slot):
        when_partner(pair, lambda: pair_copy(slot).wait_send())

        def send():
            pair_copy(slot).wait_recv()
            for peer in x_peers:
                x_send[slot, peer] = (pair_own[slot, peer] + pair_recv[slot, peer].astype(f32)).astype(bf16)
                x_copy(slot, peer, me_x).start()

        when_owner(pair, send)

    def gated(layer, group, pair, slot):
        @pl.when(pair == 0)
        def _():
            finish_squares(layer, group)

        def unit():
            total = pair_own[slot, me_x] + pair_recv[slot, me_x].astype(f32)
            for peer in x_peers:
                copy = x_copy(slot, peer, peer)
                copy.wait_send()
                copy.wait_recv()
                total = total + x_recv[slot, peer].astype(f32)
            at = (pair * CORES + me_core) * chunk_cols
            cols = pl.ds(pl.multiple_of(at, chunk_cols), chunk_cols)
            one = pl.ds(layer, 1)

            def mine(values):
                kept = values[:, :LANES]
                for x in range(1, x_count):
                    kept = jnp.where(me_x == x, values[:, x * LANES : (x + 1) * LANES], kept)
                return kept

            scales = jnp.concatenate([mine(gate_scale[one, cols]), mine(value_scale[one, cols])], axis=1)
            weights = jnp.concatenate(
                [mine(conv_gate[:, layer, cols]), mine(conv_value[:, layer, cols])], axis=1
            )
            inv = inverse[group]
            pre = total * jnp.concatenate([inv, inv], axis=1) * scales
            before = carry[pair]
            padded[:8] = jnp.where(group == 0, jnp.zeros_like(before), before)
            padded[8:] = pre
            carry[pair] = pre[rows - 8 :]
            mixed = pre * weights[taps - 1 : taps]
            for tap in range(taps - 1):
                mixed = mixed + padded[pl.ds(8 - (taps - 1) + tap, rows), :] * weights[tap : tap + 1]
            hidden[slot, me_core * x_count + me_x] = (
                jax.nn.gelu(mixed[:, :LANES], approximate=True) * mixed[:, LANES:]
            ).astype(bf16)
            for peer in x_peers:
                hx_copy(slot, peer, me_x).start()

        when_owner(pair, unit)

    def pair_gather(layer, group, pair, slot):
        def forward():
            for peer in x_peers:
                hx_copy(slot, peer, me_x).wait_send()
                hx_copy(slot, peer, peer).wait_recv()
            hp_copy(slot, me_core).start()

        when_owner(pair, forward)

    def down_ready(layer, group, pair, slot):
        first = layer * chunks + pair * CORES
        end = (layer + 1) * chunks

        @pl.when(group == 0)
        def _():
            for n in range(CORES):

                @pl.when(first + n < end)
                def _(n=n):
                    for copy in down_copies(first + n):
                        copy.wait()

        when_owner(pair, lambda: hp_copy(slot, me_core).wait_send())
        when_partner(pair, lambda: hp_copy(slot, 1 - me_core).wait_recv())

    def down_parts(layer, group, pair, slot):
        first = layer * chunks + pair * CORES

        def add(count):
            left = jnp.concatenate([hidden[slot, n] for n in range(count * x_count)], axis=1).astype(f32)
            right = jnp.concatenate(
                [down_weight[lax.rem(first + n, DOWN_SLOTS)] for n in range(count)], axis=0
            )
            product = jnp.dot(left, right, preferred_element_type=f32)
            before = acc[...]
            acc[...] = jnp.where(pair == 0, jnp.zeros_like(before), before) + product

        return lambda: add(CORES), lambda: add(1)

    def down_done(layer, group, pair, slot):
        first = layer * chunks + pair * CORES
        end = (layer + 1) * chunks

        @pl.when(group == groups - 1)
        def _():
            for n in range(CORES):

                @pl.when(first + n < end)
                def _(n=n):
                    start_copies(down_copies, first + n + DOWN_SLOTS, streamed)

        @pl.when(pair == pairs - 1)
        def _():
            part = layer * groups + group
            total = acc[...].reshape(ra_count, z_block, width)
            z_send[part] = total.astype(bf16)
            z_own[part] = acc[pl.ds(pl.multiple_of(me_ra * z_block, z_block), z_block), :]
            for peer in ra_peers:
                z_copy(part, peer, me_ra).start()

    def z_sum(layer, group, pair, slot):
        part = layer * groups + group
        total = z_own[part]
        for peer in ra_peers:
            copy = z_copy(part, peer, peer)
            copy.wait_send()
            copy.wait_recv()
            total = total + z_recv[part, peer].astype(f32)
        kept = residual_weight * current[layer, group, me_ra].astype(f32)
        block = (kept + down_scale[pl.ds(layer, 1), :] * total).astype(bf16)
        current[layer + 1, group, me_ra] = block
        for peer in ra_peers:
            c_copy(part, layer + 1, group, peer, me_ra).start()
        return block

    def last_sum(layer, group, pair, slot):
        wide = z_sum(layer, group, pair, slot).astype(f32)
        squares = jnp.broadcast_to(jnp.sum(wide * wide, axis=1, keepdims=True), (z_block, LANES))
        last_send[group] = jnp.concatenate([squares] * (LANES // z_block), axis=0).T[:8]
        for peer in cb_peers:
            last_copy(group, peer, me_cb).start()

    def last_squares(layer, group, pair, slot):
        total = last_send[group]
        for peer in cb_peers:
            copy = last_copy(group, peer, peer)
            copy.wait_send()
            copy.wait_recv()
            total = total + last_recv[group, peer]
        block_recv[group, me_ra] = total
        for peer in ra_peers:
            block_copy(group, peer, me_ra).start()

    def wait_blocks(layer, group):
        part = layer * groups + group
        for peer in ra_peers:
            c_copy(part, layer + 1, group, peer, me_ra).wait_send()
            c_copy(part, layer + 1, group, peer, peer).wait_recv()

    def z_gather(layer, group, pair, slot):
        wait_blocks(layer, group)
        scale_rows(layer + 1, group)
        send_squares(layer + 1, group)

    def last_gather(layer, group, pair, slot):
        wait_blocks(layer, group)
        for peer in ra_peers:
            block_copy(group, peer, me_ra).wait_send()
            block_copy(group, peer, peer).wait_recv()
        lane = lax.broadcasted_iota(jnp.int32, (8, LANES), 1)
        squares = jnp.zeros((8, LANES), f32)
        for ra_at in range(ra_count):
            inside = (lane >= ra_at * z_block) & (lane < (ra_at + 1) * z_block)
            squares = jnp.where(inside, block_recv[group, ra_at], squares)
        row = lax.rsqrt(squares / model_width + epsilon)
        inv = jnp.broadcast_to(row[:1], (LANES, LANES)).T[:rows]
        wide = current[layers, group].reshape(rows, width).astype(f32)
        inv = jnp.concatenate([inv] * (width // LANES), axis=1)
        out[group] = (wide * inv * gains[pl.ds(layers, 1), :]).astype(bf16)
        out_copy(group).start()

    def out_copy(group):
        return pltpu.make_async_copy(out.at[group], out_hbm.at[group], out_sem.at[group])

    def last_copy(group, peer, source):
        return remote(
            last_send.at[group], last_recv.at[group, source], last_ss.at[group, peer], last_rs.at[group, source], "cb", peer
        )

    def block_copy(group, peer, source):
        place = block_recv.at[group, source]
        return remote(place, place, block_ss.at[group, peer], block_rs.at[group, source], "ra", peer)

    stages = (
        (DOWN + LAST_GATHER, "last", last_gather),
        (DOWN + LAST_SQUARES, "last", last_squares),
        (DOWN + LAST_SUM, "last", last_sum),
        (DOWN + Z_GATHER, "inner", z_gather),
        (DOWN + Z_SUM, "inner", z_sum),
        (PAIR_GATHER, "", pair_gather),
        (GATED, "", gated),
    )
    late_stages = ((PAIR_SUM, "", pair_sum),)

    delays = sorted({delay for delay, _, _ in stages + late_stages} | {0, DOWN})

    def started(delay):
        layer, rest = divmod(-delay, period)
        group, pair = (groups, rest - per_layer) if rest >= per_layer else divmod(rest, pairs)
        return tuple(jnp.int32(value) for value in (layer, group, pair, 0))

    def advanced(place):
        layer, group, pair, slot = place
        used = (layer >= 0) & (group < groups)
        slot = jnp.where(used, jnp.where(slot == RING - 1, 0, slot + 1), slot)
        wrap = pair + 1 == jnp.where(group == groups, BUBBLES, pairs)
        pair = jnp.where(wrap, 0, pair + 1)
        group = jnp.where(wrap, group + 1, group)
        next_layer = group == all_groups
        return jnp.where(next_layer, layer + 1, layer), jnp.where(next_layer, 0, group), pair, slot

    def multiply(wide_place, down_place):
        def valid(place):
            return (place[0] >= 0) & (place[0] < layers) & (place[1] < groups)

        def full(place):
            return place[2] < pairs - chunks % CORES

        wide_on, down_on = valid(wide_place), valid(down_place)
        merged = wide_on & down_on & full(wide_place) & full(down_place)
        pl.when(wide_on)(lambda: project_ready(*wide_place))
        pl.when(down_on)(lambda: down_ready(*down_place))

        @pl.when(merged)
        def _():
            project_parts(*wide_place)[0]()
            down_parts(*down_place)[0]()

        @pl.when(wide_on & jnp.logical_not(merged))
        def _():
            when_full(wide_place[2], *project_parts(*wide_place))

        @pl.when(down_on & jnp.logical_not(merged))
        def _():
            when_full(down_place[2], *down_parts(*down_place))

        @pl.when(wide_on)
        def _():
            when_partner(wide_place[2], lambda: pair_copy(wide_place[3]).start())
            project_done(*wide_place)

        pl.when(down_on)(lambda: down_done(*down_place))

    def step(index, places):
        run_stages(stages, places)
        multiply(places[delays.index(0)], places[delays.index(DOWN)])
        run_stages(late_stages, places)
        return tuple(advanced(place) for place in places)

    def run_stages(chosen, places):
        for delay, ending, stage in chosen:
            place = places[delays.index(delay)]
            layer, group, pair, slot = place
            valid = (layer >= 0) & (layer < layers) & (group < groups)
            if ending:
                valid = valid & (pair == pairs - 1) & ((layer == layers - 1) == (ending == "last"))

            @pl.when(valid)
            def _(stage=stage, place=place):
                stage(*place)

    lax.fori_loop(0, last_item + DOWN + LAST_GATHER, step, tuple(started(delay) for delay in delays))
    for group in range(groups):
        out_copy(group).wait()


def fits(ra_count, cb_count, tokens, gate_weight, conv_gate):
    rows, width = tokens.shape
    layers, _, units = gate_weight.shape
    if cb_count % CORES or cb_count <= CORES or ra_count < 2 or rows % GROUP or GROUP % (16 * ra_count):
        return False
    chunk_cols = cb_count // CORES * LANES
    if width % LANES or units % chunk_cols or units // chunk_cols < CORES or conv_gate.shape[1] > 9:
        return False
    chunks = units // chunk_cols
    pairs, groups = pl.cdiv(chunks, CORES), rows // GROUP
    weights = 4 * width * chunk_cols * (2 * WIDE_SLOTS + DOWN_SLOTS)
    return (
        chunks <= min(WIDE_SLOTS, DOWN_SLOTS)
        and (groups - 1) * pairs + 1 + BUBBLES >= DOWN + Z_GATHER
        and weights + 4 * rows * width * 12 <= 60 * 1024 * 1024
    )


def on_device_any(ra_count, cb_count, *args):
    (
        tokens,
        norm_gains,
        gate_weight,
        value_weight,
        gate_scale,
        value_scale,
        conv_gate,
        conv_value,
        down_weight,
        down_scale,
    ) = args
    if not fits(ra_count, cb_count, tokens, gate_weight, conv_gate):
        return on_device(*args)
    f32, bf16 = jnp.float32, jnp.bfloat16
    layers, width, units = gate_weight.shape
    groups, rows = tokens.shape[0] // GROUP, GROUP
    x_count = cb_count // CORES
    chunk_cols = x_count * LANES
    pairs = pl.cdiv(units // chunk_cols, CORES)
    z_block = rows // ra_count
    parts, events = layers * groups, layers * groups
    vmem, dma = pltpu.VMEM, pltpu.SemaphoreType.DMA
    in_hbm = pl.BlockSpec(memory_space=pl.ANY)
    taps = conv_gate.shape[1]
    result = pl.pallas_call(
        functools.partial(fused_kernel, ra_count, cb_count),
        out_shape=jax.ShapeDtypeStruct((groups, rows, width), bf16),
        in_specs=[in_hbm] * 10,
        out_specs=in_hbm,
        scratch_shapes=[
            vmem(norm_gains.shape, f32),
            vmem(gate_scale.shape, f32),
            vmem(value_scale.shape, f32),
            vmem((taps, layers, units), f32),
            vmem((taps, layers, units), f32),
            vmem(down_scale.shape, f32),
            vmem((groups, rows, width), bf16),
            vmem((WIDE_SLOTS, width, 2 * chunk_cols), f32),
            vmem((DOWN_SLOTS, chunk_cols, width), f32),
            vmem((layers + 1, groups, ra_count, z_block, width), bf16),
            vmem((groups, rows, width), f32),
            vmem((groups, rows, LANES), f32),
            vmem((rows + 8, 2 * LANES), f32),
            vmem((pairs, 8, 2 * LANES), f32),
            vmem((RING, x_count, rows, 2 * LANES), bf16),
            vmem((RING, x_count, rows, 2 * LANES), bf16),
            vmem((RING, x_count, rows, 2 * LANES), f32),
            vmem((RING, x_count, rows, 2 * LANES), bf16),
            vmem((RING, x_count, rows, 2 * LANES), bf16),
            vmem((RING, cb_count, rows, LANES), bf16),
            vmem((rows, width), f32),
            vmem((parts, ra_count, z_block, width), bf16),
            vmem((parts, ra_count, z_block, width), bf16),
            vmem((parts, z_block, width), f32),
            vmem((events, 8, LANES), f32),
            vmem((events, cb_count, 8, LANES), f32),
            vmem((groups, 8, LANES), f32),
            vmem((groups, cb_count, 8, LANES), f32),
            vmem((groups, ra_count, 8, LANES), f32),
            dma((7,)),
            dma((groups,)),
            dma((WIDE_SLOTS, 2)),
            dma((DOWN_SLOTS,)),
            dma((RING,)),
            dma((RING,)),
            dma((RING, x_count)),
            dma((RING, x_count)),
            dma((RING, x_count)),
            dma((RING, x_count)),
            dma((RING,)),
            dma((RING,)),
            dma((parts, ra_count)),
            dma((parts, ra_count)),
            dma((parts, ra_count)),
            dma((parts, ra_count)),
            dma((events, cb_count)),
            dma((events, cb_count)),
            dma((groups, cb_count)),
            dma((groups, cb_count)),
            dma((groups, ra_count)),
            dma((groups, ra_count)),
        ],
        compiler_params=pltpu.CompilerParams(
            collective_id=0, has_side_effects=True, vmem_limit_bytes=67043328
        ),
        name="fused_sublayers",
    )(
        tokens.reshape(groups, ra_count, z_block, width),
        norm_gains,
        gate_weight,
        value_weight,
        gate_scale,
        value_scale,
        conv_gate.transpose(1, 0, 2),
        conv_value.transpose(1, 0, 2),
        down_weight,
        down_scale,
    )
    return result.reshape(groups * rows, width)


def solution(mesh):
    in_specs = (
        P("grp", "cb"),
        P(None, "cb"),
        P(None, "cb", "ra"),
        P(None, "cb", "ra"),
        P(None, "ra"),
        P(None, "ra"),
        P(None, None, "ra"),
        P(None, None, "ra"),
        P(None, "ra", "cb"),
        P(None, "cb"),
    )
    out_specs = P("grp", "cb")
    return jax.shard_map(
        functools.partial(on_device_any, mesh.shape["ra"], mesh.shape["cb"]), mesh=mesh, in_specs=in_specs, out_specs=out_specs, check_vma=False
    )
```
